32 devices in a mesh: ep: 4 (over y, x), tp: 8 (over z, core).
Axes of the slice: x: 2, y: 2, z: 4, core: 2. Of those that a mesh axis runs over, the one named last changes fastest.
Arguments:
- tokens: bfloat16 [256, 4096], P('ep'), may hold values from -6 to 6
- norm_gain: float32 [4096], replicated, may hold values from 0.1 to 1.9
- ffn_gain: float32 [4096], replicated, may hold values from 0.1 to 1.9
- w_in: bfloat16 [4096, 2048], P(None, 'tp'), may hold values from -0.09375 to 0.09375
- decay_rate: float32 [8192], P('tp'), may hold values from 0.02 to 2
- frequency: float32 [8192], P('tp'), may hold values from -3.140625 to 3.140625
- log_step: float32 [128], P('tp'), may hold values from -2.3 to 0
- input_real: float32 [16, 8192], P(None, 'tp'), may hold values from -1 to 1
- input_imag: float32 [16, 8192], P(None, 'tp'), may hold values from -1 to 1
- readout_real: float32 [16, 8192], P(None, 'tp'), may hold values from -0.5 to 0.5
- readout_imag: float32 [16, 8192], P(None, 'tp'), may hold values from -0.5 to 0.5
- skip_gain: float32 [2048], P('tp'), may hold values from -4 to 4
- state_real: float32 [256, 8192], P('ep', 'tp'), may hold values from -6 to 6
- state_imag: float32 [256, 8192], P('ep', 'tp'), may hold values from -6 to 6
- w_out: bfloat16 [2048, 4096], P('tp'), may hold values from -0.125 to 0.125
- shared_gate: bfloat16 [4096, 1024], P(None, 'tp'), may hold values from -0.09375 to 0.09375
- shared_up: bfloat16 [4096, 1024], P(None, 'tp'), may hold values from -0.09375 to 0.09375
- shared_down: bfloat16 [1024, 4096], P('tp'), may hold values from -0.1875 to 0.1875
- expert_gate: bfloat16 [16, 4096, 1024], P('ep', 'tp'), may hold values from -0.09375 to 0.09375
- expert_up: bfloat16 [16, 4096, 1024], P('ep', 'tp'), may hold values from -0.09375 to 0.09375
- expert_down: bfloat16 [16, 1024, 4096], P('ep', None, 'tp'), may hold values from -0.1875 to 0.1875
- routing: int32 [256, 4], P('ep'), may hold values from 0 to 15, all different within a row; in each aligned block of 64 rows (0 to 63, 64 to 127, ...) at most 32 rows name the same one
- route_weight: float32 [256, 4], P('ep'), may hold values from 0.1 to 1
Outputs:
- mixed: bfloat16 [256, 4096], P('ep', 'tp')
- new_state_real: float32 [256, 8192], P('ep', 'tp')
- new_state_imag: float32 [256, 8192], P('ep', 'tp')
The draws below stay inside these ranges and needn't reach their ends.
Inputs may be any that keep to these rules, and one draw needn't show every extreme that they name: `routing`: each row names 4 different experts. In the rows of one index of ep (aligned blocks of 64 rows) no expert is named more than 32 times, and in every draw some expert is named exactly 32 times in some block.
All inputs are finite; a program needn't handle non-finite values.
Results may differ from the reference program's by a relative error of at most 0.02.
Values may be sent and summed in bfloat16 or wider, within the bound.
A program may use at most 64 MiB of HBM per device.

```python
import math
import jax
import jax.numpy as jnp
import numpy as np
from jax import lax

D = 4096
GROUPS = 128
CHAN = 16
STATE = 64
FE = 1024
FS = 1024
TOP_K = 4
SEQ_DEV = 64
SEQS = 256
EXPERTS = 16
CAP = 32


def steps_of(rng, dims, pieces, low, high):
    loudness, own = 1.0, jax.random.fold_in(rng, 6)
    for axis_at, shards_of in pieces:
        heights = jnp.exp(jax.random.uniform(jax.random.fold_in(own, axis_at), (shards_of,), jnp.float32, low / len(pieces), high / len(pieces)))
        loudness = loudness * jnp.repeat(heights, dims[axis_at] // shards_of).reshape([-1 if axis == axis_at else 1 for axis in range(len(dims))])
    return loudness


def routed_block(key, own, number, rows, amount, top, most, skew):
    sequence = jax.random.permutation(key, amount)
    heavy_load, usual = load_shares(amount, rows * top, most, skew, True), load_shares(amount, rows * top, most, skew, False)
    places = jnp.arange(amount)

    def named(tallies, rotation):
        used = int((tallies > 0).sum())
        fixed = max(1, used // 4)
        shifted = fixed + (places - fixed + rotation * (used - fixed)) % max(1, amount - fixed)
        return jnp.zeros((amount,), jnp.int32).at[sequence[jnp.where(places < fixed, places, shifted)]].set(jnp.asarray(tallies, jnp.int32))

    tallies = jnp.where(number % 4 == 0, named(heavy_load, number // 4), named(usual, number - number // 4 - 1))
    mixed = jax.random.permutation(jax.random.fold_in(own, 3), amount)
    source_of, taker = mixed[0:amount // 2 * 2:2], mixed[1:amount // 2 * 2:2]
    margin = jnp.minimum(tallies[source_of] - 1, most - tallies[taker]) // 2
    margin = jnp.where((source_of == sequence[0]) | (taker == sequence[0]) | (tallies[taker] == 0), 0, jnp.maximum(margin, 0))
    shifted = jax.random.randint(jax.random.fold_in(own, 4), (amount // 2,), 0, 1 << 20) % (margin + 1)
    tallies = tallies.at[source_of].add(-shifted).at[taker].add(shifted)
    members = jnp.searchsorted(jnp.cumsum(tallies), jnp.arange(rows * top), side="right").astype(jnp.int32)
    table = members.reshape(top, rows).T
    table = table[jax.random.permutation(jax.random.fold_in(own, 1), rows)]
    rotation = jax.random.randint(jax.random.fold_in(own, 2), (rows, 1), 0, top)
    return jnp.take_along_axis(table, (jnp.arange(top)[None, :] + rotation) % top, axis=1)


def load_shares(count, total, bound, skew, full):
    loads = [(1 << 20) // math.isqrt(standing ** skew) + 1 for standing in range(1, count + 1)]
    largest = bound if full else min(bound, max(-(-total // count), total * loads[0] // sum(loads)))
    least = 1 if total - largest >= count - 1 else 0
    holding, spare = [largest] + [least] * (count - 1), total - largest - least * (count - 1)
    while spare > 0:
        free = [i for i in range(1, count) if holding[i] < largest] or [i for i in range(1, count) if holding[i] < bound]
        mass, budget = sum([loads[i] for i in free]), spare
        for i in free:
            more = min(bound - holding[i], max(1, budget * loads[i] // mass), spare)
            holding[i] = holding[i] + more
            spare = spare - more
    return np.array(holding)


def noise(own_key, dims, scale, reach, pieces=(), kind=jnp.bfloat16):
    entries = jax.random.normal(own_key, dims, jnp.float32) * scale
    if len(pieces) > 0:
        entries = steps_of(own_key, dims, pieces, -0.22, 0.18) * entries
    return jnp.clip(entries, min=-reach, max=reach).astype(kind)


def setup_inputs(seed: int = 0) -> dict:
    streams_of = jax.random.split(jax.random.key(seed), 24)
    tokens = noise(streams_of[0], (SEQS, D), 1.0, 6.0, ((0, 4),))
    norm_gain = jnp.clip(1.0 + 0.18 * jax.random.normal(streams_of[1], (D,), jnp.float32), 0.1, 1.9)
    ffn_gain = jnp.clip(1.0 + 0.18 * jax.random.normal(streams_of[2], (D,), jnp.float32), 0.1, 1.9)
    w_in = noise(streams_of[3], (D, GROUPS * CHAN), D ** -0.5, 0.09375, ((1, 8),))
    decay_rate = jnp.clip(jnp.exp(math.log(2.0) - 4.6051702 * jax.random.uniform(streams_of[4], (GROUPS * STATE,), jnp.float32) ** steps_of(streams_of[4], (GROUPS * STATE,), ((0, 8),), -0.2, 0.2)), 0.02, 2.0)
    frequency = jnp.clip(jax.random.uniform(streams_of[5], (GROUPS * STATE,), jnp.float32, -3.140625, 3.140625), -3.140625, 3.140625)
    log_step = jnp.clip(-2.3 + 2.3 * jax.random.uniform(streams_of[6], (GROUPS,), jnp.float32) ** steps_of(streams_of[6], (GROUPS,), ((0, 8),), -0.2, 0.2), -2.3, 0.0)
    input_real = noise(streams_of[7], (CHAN, GROUPS * STATE), (2 * CHAN) ** -0.5, 1.0, ((1, 8),), jnp.float32)
    input_imag = noise(streams_of[8], (CHAN, GROUPS * STATE), (2 * CHAN) ** -0.5, 1.0, ((1, 8),), jnp.float32)
    readout_real = noise(streams_of[9], (CHAN, GROUPS * STATE), (2 * STATE) ** -0.5, 0.5, ((1, 8),), jnp.float32)
    readout_imag = noise(streams_of[10], (CHAN, GROUPS * STATE), (2 * STATE) ** -0.5, 0.5, ((1, 8),), jnp.float32)
    skip_gain = noise(streams_of[11], (GROUPS * CHAN,), 1.0, 4.0, ((0, 8),), jnp.float32)
    state_real = noise(streams_of[12], (SEQS, GROUPS * STATE), 1.0, 6.0, ((0, 4), (1, 8)), jnp.float32)
    state_imag = noise(streams_of[13], (SEQS, GROUPS * STATE), 1.0, 6.0, ((0, 4), (1, 8)), jnp.float32)
    w_out = noise(streams_of[14], (GROUPS * CHAN, D), (GROUPS * CHAN) ** -0.5, 0.125, ((0, 8),))
    shared_gate = noise(streams_of[15], (D, FS), D ** -0.5, 0.09375, ((1, 8),))
    shared_up = noise(streams_of[16], (D, FS), D ** -0.5, 0.09375, ((1, 8),))
    shared_down = noise(streams_of[17], (FS, D), FS ** -0.5, 0.1875, ((0, 8),))
    expert_gate = noise(streams_of[18], (EXPERTS, D, FE), D ** -0.5, 0.09375, ((0, 4), (1, 8)))
    expert_up = noise(streams_of[19], (EXPERTS, D, FE), D ** -0.5, 0.09375, ((0, 4), (1, 8)))
    expert_down = noise(streams_of[20], (EXPERTS, FE, D), FE ** -0.5, 0.1875, ((0, 4), (2, 8)))
    routing_keys = jax.random.split(jax.random.fold_in(streams_of[21], 1), SEQS // SEQ_DEV)
    routing_turns = jax.random.permutation(jax.random.fold_in(streams_of[21], 3), SEQS // SEQ_DEV)
    routing = jax.vmap(lambda own, number: routed_block(jax.random.fold_in(streams_of[21], 2), own, number, SEQ_DEV, EXPERTS, TOP_K, CAP, 2))(routing_keys, routing_turns).reshape((SEQS, TOP_K))
    route_weight = jnp.clip(jnp.exp(math.log(1.0) - 2.3025851 * jax.random.uniform(streams_of[22], (SEQS, TOP_K), jnp.float32) ** steps_of(streams_of[22], (SEQS, TOP_K), ((0, 4),), -0.2, 0.2)), 0.1, 1.0)
    return {"tokens": tokens, "norm_gain": norm_gain, "ffn_gain": ffn_gain, "w_in": w_in, "decay_rate": decay_rate, "frequency": frequency, "log_step": log_step, "input_real": input_real, "input_imag": input_imag, "readout_real": readout_real, "readout_imag": readout_imag, "skip_gain": skip_gain, "state_real": state_real, "state_imag": state_imag, "w_out": w_out, "shared_gate": shared_gate, "shared_up": shared_up, "shared_down": shared_down, "expert_gate": expert_gate, "expert_up": expert_up, "expert_down": expert_down, "routing": routing, "route_weight": route_weight}


EPS = 1e-06
ROUTED_SCALE = 2.5
HIGH = lax.Precision.HIGHEST

def rms_scale(values_in, gains):
    values = values_in.astype(jnp.float32)
    factor = lax.rsqrt(lax.optimization_barrier(jnp.mean(values * values, axis=-1, keepdims=True)) + EPS)
    return (values * factor * gains).astype(jnp.bfloat16)

def state_update(normed, w_in, decay_rate, frequency, log_step, input_real, input_imag, readout_real, readout_imag, skip_gain, state_real, state_imag):
    seq_count = normed.shape[0]
    groups = log_step.shape[0]
    chan_count = skip_gain.shape[0] // groups
    state_width = decay_rate.shape[0] // groups
    drive_rows = jnp.dot(normed, w_in, preferred_element_type=jnp.float32).astype(jnp.bfloat16)
    drive_f = drive_rows.astype(jnp.float32).reshape(seq_count, groups, chan_count)
    decays = decay_rate.reshape(groups, state_width)
    omegas = frequency.reshape(groups, state_width)
    step_size = jnp.exp(log_step)[:, None]
    pole_mag = jnp.exp(-decays * step_size)
    pole_angle = omegas * step_size
    pole_re = pole_mag * jnp.cos(pole_angle)
    pole_im = pole_mag * jnp.sin(pole_angle)
    pole_norm = decays * decays + omegas * omegas
    diff_re = pole_re - 1.0
    lift_re = (-decays * diff_re + omegas * pole_im) / pole_norm
    lift_im = (-decays * pole_im - omegas * diff_re) / pole_norm
    in_re = input_real.reshape(chan_count, groups, state_width)
    in_im = input_imag.reshape(chan_count, groups, state_width)
    push_re = jnp.einsum('sgh,hgp->sgp', drive_f, in_re, precision=HIGH)
    push_im = jnp.einsum('sgh,hgp->sgp', drive_f, in_im, precision=HIGH)
    old_re = state_real.reshape(seq_count, groups, state_width)
    old_im = state_imag.reshape(seq_count, groups, state_width)
    new_re = pole_re * old_re - pole_im * old_im + lift_re * push_re - lift_im * push_im
    new_im = pole_re * old_im + pole_im * old_re + lift_re * push_im + lift_im * push_re
    out_re = readout_real.reshape(chan_count, groups, state_width)
    out_im = readout_imag.reshape(chan_count, groups, state_width)
    read_rows = jnp.einsum('sgp,hgp->sgh', new_re, out_re, precision=HIGH) - jnp.einsum('sgp,hgp->sgh', new_im, out_im, precision=HIGH)
    read_rows = read_rows + skip_gain.reshape(groups, chan_count) * drive_f
    activated = jax.nn.gelu(read_rows).reshape(seq_count, groups * chan_count).astype(jnp.bfloat16)
    return (activated, new_re.reshape(seq_count, groups * state_width), new_im.reshape(seq_count, groups * state_width))

def reference(tokens, norm_gain, ffn_gain, w_in, decay_rate, frequency, log_step, input_real, input_imag, readout_real, readout_imag, skip_gain, state_real, state_imag, w_out, shared_gate, shared_up, shared_down, expert_gate, expert_up, expert_down, routing, route_weight):
    normed = rms_scale(tokens, norm_gain)
    activated, new_real, new_imag = state_update(normed, w_in, decay_rate, frequency, log_step, input_real, input_imag, readout_real, readout_imag, skip_gain, state_real, state_imag)
    mixer_terms = jnp.dot(activated, w_out, preferred_element_type=jnp.float32)
    resid = (tokens.astype(jnp.float32) + mixer_terms).astype(jnp.bfloat16)
    ffn_rows = rms_scale(resid, ffn_gain)
    shared_gate_rows = jnp.dot(ffn_rows, shared_gate, preferred_element_type=jnp.float32)
    shared_up_rows = jnp.dot(ffn_rows, shared_up, preferred_element_type=jnp.float32)
    shared_inner = (jax.nn.silu(shared_gate_rows) * shared_up_rows).astype(jnp.bfloat16)
    shared = jnp.dot(shared_inner, shared_down, preferred_element_type=jnp.float32)
    seq_total = tokens.shape[0]
    expert_count = expert_gate.shape[0]
    block_count = seq_total // SEQ_DEV
    per_block = SEQ_DEV * TOP_K
    flat_ids = routing.reshape(-1).astype(jnp.int32)
    one_hot = (flat_ids[:, None] == jnp.arange(expert_count, dtype=jnp.int32)[None, :]).astype(jnp.int32)
    blocked = one_hot.reshape(block_count, per_block, expert_count)
    earlier = (jnp.cumsum(blocked, axis=1) - blocked).reshape(seq_total * TOP_K, expert_count)
    slot_rank = lax.optimization_barrier(jnp.sum(earlier * one_hot, axis=1)).astype(jnp.int32)
    block_ids = (jnp.arange(seq_total * TOP_K, dtype=jnp.int32) // per_block).astype(jnp.int32)
    buffer_rows = block_count * CAP
    column = (block_ids * CAP + slot_rank).astype(jnp.int32)
    token_ids = (jnp.arange(seq_total * TOP_K, dtype=jnp.int32) // TOP_K).astype(jnp.int32)
    table = jnp.full((expert_count, buffer_rows), seq_total, jnp.int32).at[flat_ids, column].set(token_ids)
    padded = jnp.concatenate([ffn_rows, jnp.zeros((1, ffn_rows.shape[1]), jnp.bfloat16)], axis=0)

    def one_expert(args):
        index_rows, gate_w, up_w, down_w = args
        picked = padded[index_rows].astype(jnp.float32)
        gate_rows = jnp.dot(picked, gate_w.astype(jnp.float32), preferred_element_type=jnp.float32)
        up_rows = jnp.dot(picked, up_w.astype(jnp.float32), preferred_element_type=jnp.float32)
        inner_rows = (jax.nn.silu(gate_rows) * up_rows).astype(jnp.bfloat16)
        return jnp.dot(inner_rows.astype(jnp.float32), down_w.astype(jnp.float32), preferred_element_type=jnp.float32)
    outputs = lax.map(one_expert, (table, expert_gate, expert_up, expert_down))
    flat_out = outputs.reshape(expert_count * buffer_rows, outputs.shape[2])
    picked_rows = flat_out[(flat_ids * buffer_rows + column).astype(jnp.int32)].reshape(seq_total, TOP_K, outputs.shape[2])
    weights = route_weight / lax.optimization_barrier(jnp.sum(route_weight, axis=1, keepdims=True)) * ROUTED_SCALE
    routed = lax.optimization_barrier(jnp.sum(weights[:, :, None] * picked_rows, axis=1))
    mixed = (resid.astype(jnp.float32) + shared + routed).astype(jnp.bfloat16)
    return (mixed, new_real, new_imag)
```

```python
import functools

import jax
import jax.numpy as jnp
from jax import lax
from jax.experimental import pallas as pl
from jax.experimental.pallas import tpu as pltpu
from jax.sharding import PartitionSpec as P

EPS = 1e-06
ROUTED_SCALE = 2.5
F32 = jnp.float32
BF16 = jnp.bfloat16
VMEM_LIMIT = 60 * 1024 * 1024
MESH_ID = pl.DeviceIdType.MESH
IN_VMEM = pl.BlockSpec(memory_space=pltpu.VMEM)


def shift_of(size):
    assert size & (size - 1) == 0
    return size.bit_length() - 1


def split_index(shape, axis, size):
    places = lax.broadcasted_iota(jnp.int32, shape, axis)
    return lax.shift_right_logical(places, shift_of(size))


def mixer_kernel(
    tokens_ref,
    gain_ref,
    w_in_ref,
    decay_ref,
    freq_ref,
    logstep_ref,
    in_re_ref,
    in_im_ref,
    out_re_ref,
    out_im_ref,
    skip_ref,
    old_re_ref,
    old_im_ref,
    w_out_ref,
    terms_ref,
    new_re_ref,
    new_im_ref,
    *,
    groups,
):
    tokens = tokens_ref[...].astype(F32)
    factor = lax.rsqrt(jnp.mean(tokens * tokens, axis=-1, keepdims=True) + EPS)
    normed = (tokens * factor * gain_ref[...]).astype(BF16)
    drive = jnp.dot(normed, w_in_ref[...], preferred_element_type=F32).astype(BF16)
    chan = in_re_ref.shape[0]
    width = decay_ref.shape[1] // groups
    wide = (groups * chan, groups * width)
    own_group = split_index(wide, 0, chan) == split_index(wide, 1, width)

    def spread(ref):
        tiled = jnp.concatenate([ref[...]] * groups, axis=0)
        return jnp.where(own_group, tiled, 0.0).astype(BF16)

    decay, freq = decay_ref[...], freq_ref[...]
    step = jnp.exp(logstep_ref[...])
    mag = jnp.exp(-decay * step)
    pole_re = mag * jnp.cos(freq * step)
    pole_im = mag * jnp.sin(freq * step)
    norm = decay * decay + freq * freq
    diff = pole_re - 1.0
    lift_re = (-decay * diff + freq * pole_im) / norm
    lift_im = (-decay * pole_im - freq * diff) / norm
    push_re = jnp.dot(drive, spread(in_re_ref), preferred_element_type=F32)
    push_im = jnp.dot(drive, spread(in_im_ref), preferred_element_type=F32)
    old_re, old_im = old_re_ref[...], old_im_ref[...]
    new_re = pole_re * old_re - pole_im * old_im + lift_re * push_re - lift_im * push_im
    new_im = pole_re * old_im + pole_im * old_re + lift_re * push_im + lift_im * push_re
    new_re_ref[...] = new_re
    new_im_ref[...] = new_im
    nt = (((1,), (1,)), ((), ()))
    read = lax.dot_general(
        new_re.astype(BF16), spread(out_re_ref), nt, preferred_element_type=F32
    ) - lax.dot_general(new_im.astype(BF16), spread(out_im_ref), nt, preferred_element_type=F32)
    read = read + skip_ref[...] * drive.astype(F32)
    activated = jax.nn.gelu(read).astype(BF16)
    terms_ref[...] = jnp.dot(activated, w_out_ref[...], preferred_element_type=F32).astype(BF16)


def enter(tp, ep, partner, same_core, ep_peers):
    barrier = pltpu.get_barrier_semaphore()
    peers = [{"tp": d} for d in [partner] + same_core] + [{"ep": d} for d in ep_peers]
    for peer in peers:
        pl.semaphore_signal(barrier, inc=1, device_id=peer, device_id_type=MESH_ID)
    pl.semaphore_wait(barrier, len(peers))


def remote(src, dst, send_sem, recv_sem, peer):
    return pltpu.make_async_remote_copy(
        src_ref=src,
        dst_ref=dst,
        send_sem=send_sem,
        recv_sem=recv_sem,
        device_id=peer,
        device_id_type=MESH_ID,
    )


def places(tp_count, ep_count):
    tp, ep = lax.axis_index("tp"), lax.axis_index("ep")
    chips = tp_count // 2
    chip, core = tp // 2, tp % 2
    partner = chip * 2 + (1 - core)
    chip_at = [(chip + d) % chips for d in range(chips)]
    ep_at = [(ep + d) % ep_count for d in range(ep_count)]
    return tp, ep, chip, core, partner, chip_at, ep_at


def scatter_sum(block_of, mate, half, far, sems, where):
    tp, core, partner, chip_at = where
    s1, r1, s2, r2 = sems
    chips = len(chip_at)
    order = list(range(1, chips)) + [0]
    first = {}
    for d in order:
        first[d] = remote(
            block_of(chip_at[d] * 2 + (1 - core)),
            mate.at[d],
            s1.at[d],
            r1.at[d],
            {"tp": partner},
        )
        first[d].start()
    second = {}
    for d in order:
        first[d].wait_recv()
        own = block_of(chip_at[d] * 2 + core)[...].astype(F32) + mate[d].astype(F32)
        half[d] = own.astype(BF16)
        if d:
            second[d] = remote(
                half.at[d], far.at[d], s2.at[d], r2.at[d], {"tp": chip_at[d] * 2 + core}
            )
            second[d].start()

    def finish():
        for d in order:
            first[d].wait_send()
        for d in range(1, chips):
            second[d].wait()

    return finish


def gather_start(own, store, sems, where):
    tp, core, partner, chip_at = where
    s1, r1, s2, r2 = sems
    chips = len(chip_at)
    sends = []
    for d in range(1, chips):
        copy = remote(own, store(tp), s1.at[d], r1.at[d], {"tp": chip_at[d] * 2 + core})
        copy.start()
        sends.append(copy)
    mine = remote(own, store(tp), s2.at[0], r2.at[0], {"tp": partner})
    mine.start()

    def finish():
        passed = [mine]
        for d in range(1, chips):
            sends[d - 1].wait_recv()
            source = chip_at[chips - d] * 2 + core
            onward = remote(store(source), store(source), s2.at[d], r2.at[d], {"tp": partner})
            onward.start()
            passed.append(onward)
        for copy in sends:
            copy.wait_send()
        for copy in passed:
            copy.wait()

    return finish


def resid_kernel(
    terms_ref,
    tokens_ref,
    gain_ref,
    meta_ref,
    ffn_ref,
    resid_ref,
    rows_ref,
    metas_ref,
    mate,
    half,
    far,
    full,
    rows,
    metas,
    rs_s1,
    rs_r1,
    rs_s2,
    rs_r2,
    ag_s1,
    ag_r1,
    ag_s2,
    ag_r2,
    ep_s,
    ep_r,
    meta_s,
    meta_r,
    *,
    tp_count,
    ep_count,
):
    tp, ep, chip, core, partner, chip_at, ep_at = places(tp_count, ep_count)
    enter(tp, ep, partner, [c * 2 + core for c in chip_at[1:]], ep_at[1:])
    where = (tp, core, partner, chip_at)
    slice_width = rows.shape[2]

    def columns(ref):
        return lambda j: ref.at[:, pl.ds(pl.multiple_of(j * slice_width, 128), slice_width)]

    meta_copies = []
    for d in range(1, ep_count):
        copy = remote(meta_ref, metas.at[ep], meta_s.at[d], meta_r.at[d], {"ep": ep_at[d]})
        copy.start()
        meta_copies.append(copy)
    finish = scatter_sum(columns(terms_ref), mate, half, far, (rs_s1, rs_r1, rs_s2, rs_r2), where)
    finish()
    total = half[0].astype(F32)
    for d in range(1, len(chip_at)):
        total = total + far[d].astype(F32)
    resid = (columns(tokens_ref)(tp)[...].astype(F32) + total).astype(BF16)
    resid_ref[...] = resid
    columns(full)(tp)[...] = resid
    gather_start(columns(full)(tp), columns(full), (ag_s1, ag_r1, ag_s2, ag_r2), where)()
    whole = full[...].astype(F32)
    factor = lax.rsqrt(jnp.mean(whole * whole, axis=-1, keepdims=True) + EPS)
    gain_own = columns(gain_ref)(tp)[...]
    rows[ep] = (resid.astype(F32) * factor * gain_own).astype(BF16)
    row_copies = []
    for d in range(1, ep_count):
        copy = remote(rows.at[ep], rows.at[ep], ep_s.at[d], ep_r.at[d], {"ep": ep_at[d]})
        copy.start()
        row_copies.append(copy)
    ffn_ref[...] = (whole * factor * gain_ref[...]).astype(BF16)
    metas[ep] = meta_ref[...]
    for copy in meta_copies + row_copies:
        copy.wait()
    rows_ref[...] = rows[...]
    metas_ref[...] = metas[...]


def slot_map(meta_ref, row, block, base, slots, cap, seqs, values):
    shape = (slots, meta_ref.shape[1])
    slot = lax.broadcasted_iota(jnp.int32, shape, 0)
    same = lax.shift_right_logical(slot, shift_of(cap)) == split_index(shape, 1, seqs)
    wanted = ((slot & (cap - 1)) + base).astype(F32)
    total = jnp.zeros(shape, F32)
    for k in range(row):
        total = total + jnp.where(meta_ref[k : k + 1, :] == wanted, values(k), 0.0)
    return jnp.where(same, total, 0.0)


def up_kernel(meta_ref, rows_ref, gate_ref, up_ref, out_ref, *, top, cap, seqs, width):
    base = pl.program_id(0) * cap
    slots = out_ref.shape[0]
    chosen = slot_map(meta_ref, top, 0, base, slots, cap, seqs, lambda k: 1.0).astype(BF16)
    picked = jnp.dot(chosen, rows_ref[...], preferred_element_type=F32).astype(BF16)
    out_ref[:, :width] = jnp.dot(picked, gate_ref[0], preferred_element_type=F32).astype(BF16)
    out_ref[:, width:] = jnp.dot(picked, up_ref[0], preferred_element_type=F32).astype(BF16)


def down_kernel(meta_ref, inner_ref, down_ref, out_ref, total, *, top, cap, seqs):
    expert = pl.program_id(0)
    slots = inner_ref.shape[0]
    mix = slot_map(
        meta_ref, top, 0, expert * cap, slots, cap, seqs, lambda k: meta_ref[top + k : top + k + 1, :]
    ).astype(BF16)
    terms = jnp.dot(inner_ref[...], down_ref[0], preferred_element_type=F32).astype(BF16)
    part = lax.dot_general(mix, terms, (((0,), (0,)), ((), ())), preferred_element_type=F32)

    @pl.when(expert == 0)
    def _():
        total[...] = part

    @pl.when(expert > 0)
    def _():
        total[...] += part

    out_ref[...] = total[...].astype(BF16)


def inner_kernel(
    parts_ref,
    inner_ref,
    mate,
    half,
    far,
    full,
    rs_s1,
    rs_r1,
    rs_s2,
    rs_r2,
    ag_s1,
    ag_r1,
    ag_s2,
    ag_r2,
    *,
    tp_count,
    ep_count,
):
    tp, ep, chip, core, partner, chip_at, ep_at = places(tp_count, ep_count)
    enter(tp, ep, partner, [c * 2 + core for c in chip_at[1:]], [])
    where = (tp, core, partner, chip_at)
    finish = scatter_sum(
        lambda j: parts_ref.at[j], mate, half, far, (rs_s1, rs_r1, rs_s2, rs_r2), where
    )
    finish()
    total = half[0].astype(F32)
    for d in range(1, len(chip_at)):
        total = total + far[d].astype(F32)
    width = full.shape[2]
    gate, up = total[:, :width], total[:, width:]
    full[tp] = (gate / (1.0 + jnp.exp(-gate)) * up).astype(BF16)
    gather_start(full.at[tp], lambda j: full.at[j], (ag_s1, ag_r1, ag_s2, ag_r2), where)()
    inner_ref[...] = full[...]


def mixed_kernel(
    routed_ref,
    shared_ref,
    resid_ref,
    mixed_ref,
    back,
    mate,
    half,
    far,
    rs_s1,
    rs_r1,
    rs_s2,
    rs_r2,
    ep_s,
    ep_r,
    *,
    tp_count,
    ep_count,
):
    tp, ep, chip, core, partner, chip_at, ep_at = places(tp_count, ep_count)
    enter(tp, ep, partner, [c * 2 + core for c in chip_at[1:]], ep_at[1:])
    where = (tp, core, partner, chip_at)
    slice_width = back.shape[2]
    copies = []
    for d in range(1, ep_count):
        copy = remote(routed_ref.at[ep_at[d]], back.at[d], ep_s.at[d], ep_r.at[d], {"ep": ep_at[d]})
        copy.start()
        copies.append(copy)

    def columns(j):
        return shared_ref.at[:, pl.ds(pl.multiple_of(j * slice_width, 128), slice_width)]

    finish = scatter_sum(columns, mate, half, far, (rs_s1, rs_r1, rs_s2, rs_r2), where)
    finish()
    total = resid_ref[...].astype(F32) + half[0].astype(F32)
    for d in range(1, len(chip_at)):
        total = total + far[d].astype(F32)
    total = total + routed_ref[ep].astype(F32)
    for copy in copies:
        copy.wait()
    for d in range(1, ep_count):
        total = total + back[d].astype(F32)
    mixed_ref[...] = total.astype(BF16)


def local(
    tokens,
    norm_gain,
    ffn_gain,
    w_in,
    decay_rate,
    frequency,
    log_step,
    input_real,
    input_imag,
    readout_real,
    readout_imag,
    skip_gain,
    state_real,
    state_imag,
    w_out,
    shared_gate,
    shared_up,
    shared_down,
    expert_gate,
    expert_up,
    expert_down,
    routing,
    route_weight,
):
    seq_count, model_width = tokens.shape
    tp_count = lax.axis_size("tp")
    ep_count = lax.axis_size("ep")
    chips = tp_count // 2
    slice_width = model_width // tp_count
    groups = log_step.shape[0]
    modes = decay_rate.shape[0]
    expert_dev, _, hidden = expert_gate.shape
    expert_count = expert_dev * ep_count
    top_count = routing.shape[1]
    capacity = 2 * seq_count * top_count // expert_count
    slots = ep_count * capacity
    slot_count = expert_dev * slots
    own_slots = slot_count // tp_count
    dma = pltpu.SemaphoreType.DMA
    tp_sems = [dma((chips,))] * 4
    local_params = pltpu.CompilerParams(vmem_limit_bytes=VMEM_LIMIT)

    def talk(number):
        return pltpu.CompilerParams(
            collective_id=number, has_side_effects=True, vmem_limit_bytes=VMEM_LIMIT
        )

    flat_ids = routing.T.reshape(-1)
    one_hot = (flat_ids[:, None] == jnp.arange(expert_count, dtype=jnp.int32)[None, :]).astype(BF16)
    count = flat_ids.shape[0]
    before = jnp.arange(count)[:, None] > jnp.arange(count)[None, :]
    earlier = jnp.dot(before.astype(BF16), one_hot, preferred_element_type=F32)
    rank = jnp.sum(earlier * one_hot.astype(F32), axis=1)
    target = (flat_ids * capacity).astype(F32) + rank
    weights = route_weight / jnp.sum(route_weight, axis=1, keepdims=True) * ROUTED_SCALE
    meta = jnp.concatenate([target.reshape(top_count, seq_count), weights.T], axis=0)

    terms, new_real, new_imag = pl.pallas_call(
        functools.partial(mixer_kernel, groups=groups),
        out_shape=(
            jax.ShapeDtypeStruct((seq_count, model_width), BF16),
            jax.ShapeDtypeStruct((seq_count, modes), F32),
            jax.ShapeDtypeStruct((seq_count, modes), F32),
        ),
        in_specs=[IN_VMEM] * 14,
        out_specs=(IN_VMEM,) * 3,
        compiler_params=local_params,
        name="mixer",
    )(
        tokens,
        norm_gain[None, :],
        w_in,
        decay_rate[None, :],
        frequency[None, :],
        jnp.repeat(log_step, modes // groups)[None, :],
        input_real,
        input_imag,
        readout_real,
        readout_imag,
        skip_gain[None, :],
        state_real,
        state_imag,
        w_out,
    )
    block = (seq_count, slice_width)
    ffn_rows, resid_own, rows_all, metas = pl.pallas_call(
        functools.partial(resid_kernel, tp_count=tp_count, ep_count=ep_count),
        out_shape=(
            jax.ShapeDtypeStruct((seq_count, model_width), BF16),
            jax.ShapeDtypeStruct(block, BF16),
            jax.ShapeDtypeStruct((ep_count,) + block, BF16),
            jax.ShapeDtypeStruct((ep_count,) + meta.shape, F32),
        ),
        in_specs=[IN_VMEM] * 4,
        out_specs=(IN_VMEM,) * 4,
        scratch_shapes=[
            pltpu.VMEM((chips,) + block, BF16),
            pltpu.VMEM((chips,) + block, BF16),
            pltpu.VMEM((chips,) + block, BF16),
            pltpu.VMEM((seq_count, model_width), BF16),
            pltpu.VMEM((ep_count,) + block, BF16),
            pltpu.VMEM((ep_count,) + meta.shape, F32),
        ]
        + tp_sems
        + tp_sems
        + [dma((ep_count,))] * 4,
        compiler_params=talk(1),
        name="resid",
    )(terms, tokens, ffn_gain[None, :], meta)

    first_slot = (lax.axis_index("ep") * (expert_dev * capacity)).astype(F32)
    flat_meta = jnp.swapaxes(metas, 0, 1).reshape(meta.shape[0], ep_count * seq_count)
    flat_meta = flat_meta - jnp.where(jnp.arange(meta.shape[0])[:, None] < top_count, first_slot, 0.0)
    whole = lambda shape: pl.BlockSpec(shape, lambda e: (0,) * len(shape))
    parts = pl.pallas_call(
        functools.partial(up_kernel, top=top_count, cap=capacity, seqs=seq_count, width=hidden),
        out_shape=jax.ShapeDtypeStruct((slot_count, 2 * hidden), BF16),
        grid=(expert_dev,),
        in_specs=[
            whole(flat_meta.shape),
            whole((ep_count * seq_count, slice_width)),
            pl.BlockSpec((1, slice_width, hidden), lambda e: (e, 0, 0)),
            pl.BlockSpec((1, slice_width, hidden), lambda e: (e, 0, 0)),
        ],
        out_specs=pl.BlockSpec((slots, 2 * hidden), lambda e: (e, 0)),
        compiler_params=local_params,
        name="gate_up",
    )(flat_meta, rows_all.reshape(ep_count * seq_count, slice_width), expert_gate, expert_up)

    inner = pl.pallas_call(
        functools.partial(inner_kernel, tp_count=tp_count, ep_count=ep_count),
        out_shape=jax.ShapeDtypeStruct((tp_count, own_slots, hidden), BF16),
        in_specs=[IN_VMEM],
        out_specs=IN_VMEM,
        scratch_shapes=[pltpu.VMEM((chips, own_slots, 2 * hidden), BF16)] * 3
        + [pltpu.VMEM((tp_count, own_slots, hidden), BF16)]
        + tp_sems
        + tp_sems,
        compiler_params=talk(2),
        name="inner",
    )(parts.reshape(tp_count, own_slots, 2 * hidden))

    shared_gate_rows = jnp.dot(ffn_rows, shared_gate, preferred_element_type=F32)
    shared_up_rows = jnp.dot(ffn_rows, shared_up, preferred_element_type=F32)
    shared_inner = (jax.nn.silu(shared_gate_rows) * shared_up_rows).astype(BF16)
    shared_terms = jnp.dot(shared_inner, shared_down, preferred_element_type=F32).astype(BF16)

    routed = pl.pallas_call(
        functools.partial(down_kernel, top=top_count, cap=capacity, seqs=seq_count),
        out_shape=jax.ShapeDtypeStruct((ep_count * seq_count, slice_width), BF16),
        grid=(expert_dev,),
        in_specs=[
            whole(flat_meta.shape),
            pl.BlockSpec((slots, hidden), lambda e: (e, 0)),
            pl.BlockSpec((1, hidden, slice_width), lambda e: (e, 0, 0)),
        ],
        out_specs=whole((ep_count * seq_count, slice_width)),
        scratch_shapes=[pltpu.VMEM((ep_count * seq_count, slice_width), F32)],
        compiler_params=local_params,
        name="down",
    )(flat_meta, inner.reshape(slot_count, hidden), expert_down)

    mixed = pl.pallas_call(
        functools.partial(mixed_kernel, tp_count=tp_count, ep_count=ep_count),
        out_shape=jax.ShapeDtypeStruct(block, BF16),
        in_specs=[IN_VMEM] * 3,
        out_specs=IN_VMEM,
        scratch_shapes=[pltpu.VMEM((ep_count,) + block, BF16)]
        + [pltpu.VMEM((chips,) + block, BF16)] * 3
        + tp_sems
        + [dma((ep_count,))] * 2,
        compiler_params=talk(3),
        name="mixed",
    )(routed.reshape((ep_count,) + block), shared_terms, resid_own)
    return (mixed, new_real, new_imag)


def solution(mesh):
    placed = (
        P("ep", None),
        P(),
        P(),
        P(None, "tp"),
        P("tp"),
        P("tp"),
        P("tp"),
        P(None, "tp"),
        P(None, "tp"),
        P(None, "tp"),
        P(None, "tp"),
        P("tp"),
        P("ep", "tp"),
        P("ep", "tp"),
        P("tp", None),
        P(None, "tp"),
        P(None, "tp"),
        P("tp", None),
        P("ep", "tp", None),
        P("ep", "tp", None),
        P("ep", None, "tp"),
        P("ep", None),
        P("ep", None),
    )
    return jax.shard_map(
        local,
        mesh=mesh,
        in_specs=placed,
        out_specs=(P("ep", "tp"), P("ep", "tp"), P("ep", "tp")),
        check_vma=False,
    )
```

```python
import functools

import jax
import jax.numpy as jnp
from jax import lax
from jax.experimental import pallas as pl
from jax.experimental.pallas import tpu as pltpu
from jax.sharding import PartitionSpec as P

EPS = 1e-06
ROUTED_SCALE = 2.5
F32 = jnp.float32
BF16 = jnp.bfloat16
VMEM_LIMIT = 20 * 1024 * 1024
MESH_ID = pl.DeviceIdType.MESH
IN_VMEM = pl.BlockSpec(memory_space=pltpu.VMEM)


def shift_of(size):
    assert size & (size - 1) == 0
    return size.bit_length() - 1


def split_index(shape, axis, size):
    places = lax.broadcasted_iota(jnp.int32, shape, axis)
    return lax.shift_right_logical(places, shift_of(size))


def mixer_kernel(
    tokens_ref,
    gain_ref,
    w_in_ref,
    decay_ref,
    freq_ref,
    logstep_ref,
    in_re_ref,
    in_im_ref,
    out_re_ref,
    out_im_ref,
    skip_ref,
    old_re_ref,
    old_im_ref,
    w_out_ref,
    ids_ref,
    share_ref,
    terms_ref,
    new_re_ref,
    new_im_ref,
    meta_ref,
    *,
    groups,
    experts,
    cap,
):
    top, seqs = ids_ref.shape
    square = (seqs, seqs)
    before = (
        lax.broadcasted_iota(jnp.int32, square, 0) < lax.broadcasted_iota(jnp.int32, square, 1)
    ).astype(BF16)
    named = lax.broadcasted_iota(jnp.int32, (experts, seqs), 0)
    taken = jnp.zeros((experts, 1), F32)
    shares = share_ref[...]
    scale = ROUTED_SCALE / jnp.sum(shares, axis=0, keepdims=True)
    for k in range(top):
        ids = ids_ref[k : k + 1, :]
        hot = (named == ids).astype(F32)
        earlier = jnp.dot(hot.astype(BF16), before, preferred_element_type=F32) + taken
        rank = jnp.sum(earlier * hot, axis=0, keepdims=True)
        taken = taken + jnp.sum(hot, axis=1, keepdims=True)
        meta_ref[k : k + 1, :] = (ids * cap).astype(F32) + rank
        meta_ref[top + k : top + k + 1, :] = shares[k : k + 1, :] * scale
    tokens = tokens_ref[...].astype(F32)
    factor = lax.rsqrt(jnp.mean(tokens * tokens, axis=-1, keepdims=True) + EPS)
    normed = (tokens * factor * gain_ref[...]).astype(BF16)
    drive = jnp.dot(normed, w_in_ref[...], preferred_element_type=F32).astype(BF16)
    chan = in_re_ref.shape[0]
    width = decay_ref.shape[1] // groups
    wide = (groups * chan, groups * width)
    own_group = split_index(wide, 0, chan) == split_index(wide, 1, width)

    def spread(ref):
        tiled = jnp.concatenate([ref[...]] * groups, axis=0)
        return jnp.where(own_group, tiled, 0.0).astype(BF16)

    decay, freq = decay_ref[...], freq_ref[...]
    over = (groups, groups * width)
    member = lax.broadcasted_iota(jnp.int32, over, 0) == split_index(over, 1, width)
    column = jnp.sum(jnp.where(
        lax.broadcasted_iota(jnp.int32, (groups, groups), 0)
        == lax.broadcasted_iota(jnp.int32, (groups, groups), 1), logstep_ref[...], 0.0,
    ), axis=1, keepdims=True)
    step = jnp.exp(jnp.sum(jnp.where(member, column, 0.0), axis=0, keepdims=True))
    mag = jnp.exp(-decay * step)
    pole_re = mag * jnp.cos(freq * step)
    pole_im = mag * jnp.sin(freq * step)
    norm = decay * decay + freq * freq
    diff = pole_re - 1.0
    lift_re = (-decay * diff + freq * pole_im) / norm
    lift_im = (-decay * pole_im - freq * diff) / norm
    push_re = jnp.dot(drive, spread(in_re_ref), preferred_element_type=F32)
    push_im = jnp.dot(drive, spread(in_im_ref), preferred_element_type=F32)
    old_re, old_im = old_re_ref[...], old_im_ref[...]
    new_re = pole_re * old_re - pole_im * old_im + lift_re * push_re - lift_im * push_im
    new_im = pole_re * old_im + pole_im * old_re + lift_re * push_im + lift_im * push_re
    new_re_ref[...] = new_re
    new_im_ref[...] = new_im
    nt = (((1,), (1,)), ((), ()))
    read = lax.dot_general(
        new_re.astype(BF16), spread(out_re_ref), nt, preferred_element_type=F32
    ) - lax.dot_general(new_im.astype(BF16), spread(out_im_ref), nt, preferred_element_type=F32)
    read = read + skip_ref[...] * drive.astype(F32)
    activated = jax.nn.gelu(read).astype(BF16)
    terms_ref[...] = jnp.dot(activated, w_out_ref[...], preferred_element_type=F32).astype(BF16)


def enter(tp, ep, partner, same_core, ep_peers):
    barrier = pltpu.get_barrier_semaphore()
    peers = [{"tp": d} for d in [partner] + same_core] + [{"ep": d} for d in ep_peers]
    for peer in peers:
        pl.semaphore_signal(barrier, inc=1, device_id=peer, device_id_type=MESH_ID)
    pl.semaphore_wait(barrier, len(peers))


def remote(src, dst, send_sem, recv_sem, peer):
    return pltpu.make_async_remote_copy(
        src_ref=src,
        dst_ref=dst,
        send_sem=send_sem,
        recv_sem=recv_sem,
        device_id=peer,
        device_id_type=MESH_ID,
    )


def places(tp_count, ep_count):
    tp, ep = lax.axis_index("tp"), lax.axis_index("ep")
    chips = tp_count // 2
    chip, core = tp // 2, tp % 2
    partner = chip * 2 + (1 - core)
    chip_at = [(chip + d) % chips for d in range(chips)]
    ep_at = [(ep + d) % ep_count for d in range(ep_count)]
    return tp, ep, chip, core, partner, chip_at, ep_at


def scatter_sum(block_of, mate, half, far, sems, where):
    tp, core, partner, chip_at = where
    s1, r1, s2, r2 = sems
    chips = len(chip_at)
    order = list(range(1, chips)) + [0]
    first = {}
    for d in order:
        first[d] = remote(
            block_of(chip_at[d] * 2 + (1 - core)),
            mate.at[d],
            s1.at[d],
            r1.at[d],
            {"tp": partner},
        )
        first[d].start()
    second = {}
    return functools.partial(scatter_second, block_of, mate, half, far, sems, where, first, second)


def scatter_second(block_of, mate, half, far, sems, where, first, second):
    tp, core, partner, chip_at = where
    s1, r1, s2, r2 = sems
    chips = len(chip_at)
    order = list(range(1, chips)) + [0]
    for d in order:
        first[d].wait_recv()
        own = block_of(chip_at[d] * 2 + core)[...].astype(F32) + mate[d].astype(F32)
        half[d] = own.astype(BF16)
        if d:
            second[d] = remote(
                half.at[d], far.at[d], s2.at[d], r2.at[d], {"tp": chip_at[d] * 2 + core}
            )
            second[d].start()

    def finish():
        for d in order:
            first[d].wait_send()
        for d in range(1, chips):
            second[d].wait()

    return finish


def gather_start(own, store, sems, where):
    tp, core, partner, chip_at = where
    s1, r1, s2, r2 = sems
    chips = len(chip_at)
    sends = []
    for d in range(1, chips):
        copy = remote(own, store(tp), s1.at[d], r1.at[d], {"tp": chip_at[d] * 2 + core})
        copy.start()
        sends.append(copy)
    mine = remote(own, store(tp), s2.at[0], r2.at[0], {"tp": partner})
    mine.start()

    def finish():
        passed = [mine]
        for d in range(1, chips):
            sends[d - 1].wait_recv()
            source = chip_at[chips - d] * 2 + core
            onward = remote(store(source), store(source), s2.at[d], r2.at[d], {"tp": partner})
            onward.start()
            passed.append(onward)
        for copy in sends:
            copy.wait_send()
        for copy in passed:
            copy.wait()

    return finish


def resid_kernel(
    terms_ref,
    tokens_ref,
    gain_ref,
    meta_ref,
    ffn_ref,
    resid_ref,
    rows_ref,
    metas_ref,
    mate,
    half,
    far,
    full,
    rows,
    metas,
    rs_s1,
    rs_r1,
    rs_s2,
    rs_r2,
    ag_s1,
    ag_r1,
    ag_s2,
    ag_r2,
    ep_s,
    ep_r,
    meta_s,
    meta_r,
    *,
    tp_count,
    ep_count,
    first_step,
):
    tp, ep, chip, core, partner, chip_at, ep_at = places(tp_count, ep_count)
    enter(tp, ep, partner, [c * 2 + core for c in chip_at[1:]], ep_at[1:])
    where = (tp, core, partner, chip_at)
    slice_width = rows.shape[2]

    def columns(ref):
        return lambda j: ref.at[:, pl.ds(pl.multiple_of(j * slice_width, 128), slice_width)]

    meta_copies = []
    for d in range(1, ep_count):
        copy = remote(meta_ref, metas.at[ep], meta_s.at[d], meta_r.at[d], {"ep": ep_at[d]})
        copy.start()
        meta_copies.append(copy)
    scatter_sum(columns(terms_ref), mate, half, far, (rs_s1, rs_r1, rs_s2, rs_r2), where)()()
    total = half[0].astype(F32)
    for d in range(1, len(chip_at)):
        total = total + far[d].astype(F32)
    resid = (columns(tokens_ref)(tp)[...].astype(F32) + total).astype(BF16)
    resid_ref[...] = resid
    columns(full)(tp)[...] = resid
    gather_start(columns(full)(tp), columns(full), (ag_s1, ag_r1, ag_s2, ag_r2), where)()
    whole = full[...].astype(F32)
    factor = lax.rsqrt(jnp.mean(whole * whole, axis=-1, keepdims=True) + EPS)
    gain_own = columns(gain_ref)(tp)[...]
    rows[ep] = (resid.astype(F32) * factor * gain_own).astype(BF16)
    row_copies = []
    for d in range(1, ep_count):
        copy = remote(rows.at[ep], rows.at[ep], ep_s.at[d], ep_r.at[d], {"ep": ep_at[d]})
        copy.start()
        row_copies.append(copy)
    ffn_ref[...] = (whole * factor * gain_ref[...]).astype(BF16)
    metas[ep] = meta_ref[...]
    for copy in meta_copies + row_copies:
        copy.wait()
    rows_ref[...] = rows[...]
    flat = jnp.concatenate([metas[b] for b in range(ep_count)], axis=1)
    base = (ep * first_step).astype(F32)
    row = lax.broadcasted_iota(jnp.int32, flat.shape, 0)
    metas_ref[...] = flat - jnp.where(row < flat.shape[0] // 2, base, 0.0)


def slot_map(meta_ref, row, block, base, slots, cap, seqs, values):
    shape = (slots, meta_ref.shape[1])
    slot = lax.broadcasted_iota(jnp.int32, shape, 0)
    same = lax.shift_right_logical(slot, shift_of(cap)) == split_index(shape, 1, seqs)
    wanted = ((slot & (cap - 1)) + base).astype(F32)
    total = jnp.zeros(shape, F32)
    for k in range(row):
        total = total + jnp.where(meta_ref[k : k + 1, :] == wanted, values(k), 0.0)
    return jnp.where(same, total, 0.0)


def up_kernel(meta_ref, rows_ref, gate_ref, up_ref, out_ref, *, top, cap, seqs, width):
    base = pl.program_id(0) * cap
    slots = out_ref.shape[0]
    chosen = slot_map(meta_ref, top, 0, base, slots, cap, seqs, lambda k: 1.0).astype(BF16)
    picked = jnp.dot(chosen, rows_ref[...], preferred_element_type=F32).astype(BF16)
    out_ref[:, :width] = jnp.dot(picked, gate_ref[0], preferred_element_type=F32).astype(BF16)
    out_ref[:, width:] = jnp.dot(picked, up_ref[0], preferred_element_type=F32).astype(BF16)


def down_kernel(meta_ref, inner_ref, down_ref, out_ref, total, *, top, cap, seqs):
    expert = pl.program_id(0)
    slots = inner_ref.shape[0]
    mix = slot_map(
        meta_ref, top, 0, expert * cap, slots, cap, seqs, lambda k: meta_ref[top + k : top + k + 1, :]
    ).astype(BF16)
    terms = jnp.dot(inner_ref[...], down_ref[0], preferred_element_type=F32).astype(BF16)
    part = lax.dot_general(mix, terms, (((0,), (0,)), ((), ())), preferred_element_type=F32)

    @pl.when(expert == 0)
    def _():
        total[...] = part

    @pl.when(expert > 0)
    def _():
        total[...] += part

    out_ref[...] = total[...].astype(BF16)


def inner_kernel(
    parts_ref,
    ffn_ref,
    shared_gate_ref,
    shared_up_ref,
    shared_down_ref,
    inner_ref,
    shared_ref,
    mate,
    inbox,
    outbox,
    full,
    terms,
    s_mate,
    s_half,
    s_far,
    m_s,
    m_r,
    c_s,
    c_r,
    g_s,
    g_r,
    p_s,
    p_r,
    rs_s1,
    rs_r1,
    rs_s2,
    rs_r2,
    *,
    tp_count,
    ep_count,
):
    tp, ep, chip, core, partner, chip_at, ep_at = places(tp_count, ep_count)
    chips = tp_count // 2
    pieces = full.shape[2]
    width = full.shape[4]
    other = 1 - core
    enter(tp, ep, partner, [c * 2 + core for c in chip_at[1:]], [])
    stage = [chips - 1 - chip, chip]
    ahead = [(chip - 1) * 2 + core, (chip + 1) * 2 + core]
    back = [(chip + 1) * 2 + core, (chip - 1) * 2 + core]

    def to_mate(h, k):
        return remote(
            parts_ref.at[h, other, k], mate.at[h, k], m_s.at[h, k], m_r.at[h, k], {"tp": partner}
        )

    def to_ahead(h, k):
        return remote(
            outbox.at[h, k], inbox.at[h, k], c_s.at[h, k], c_r.at[h, k], {"tp": ahead[h]}
        )

    def to_back(h, k):
        piece = full.at[h, core, k]
        return remote(piece, piece, g_s.at[h, k], g_r.at[h, k], {"tp": back[h]})

    def to_partner(h, k):
        piece = full.at[h, core, k]
        return remote(piece, piece, p_s.at[h, k], p_r.at[h, k], {"tp": partner})

    def sum_step(h, k):
        to_mate(h, k).wait_recv()
        own = parts_ref[h, core, k].astype(F32) + mate[h, k].astype(F32)

        @pl.when(stage[h] == 0)
        def _():
            outbox[h, k] = own.astype(BF16)

        @pl.when(stage[h] > 0)
        def _():
            to_ahead(h, k).wait_recv()
            total = own + inbox[h, k].astype(F32)

            @pl.when(stage[h] < chips - 1)
            def _():
                outbox[h, k] = total.astype(BF16)

            @pl.when(stage[h] == chips - 1)
            def _():
                gate, up = total[:, :width], total[:, width:]
                full[h, core, k] = (gate / (1.0 + jnp.exp(-gate)) * up).astype(BF16)
                to_back(h, k).start()
                to_partner(h, k).start()

        @pl.when(stage[h] < chips - 1)
        def _():
            to_ahead(h, k).start()

    def pass_step(h, k):
        to_back(h, k).wait_recv()

        @pl.when(stage[h] > 0)
        def _():
            to_back(h, k).start()

        to_partner(h, k).start()

    gap = 2

    def one_step(i):
        for h in range(2):
            k = i - gap * stage[h]

            @pl.when((k >= 0) & (k < pieces))
            def _():
                sum_step(h, k)

        for h in range(2):
            late = i - gap * (chips - 1) - gap * (chips - 1 - stage[h])

            @pl.when((stage[h] < chips - 1) & (late >= 0) & (late < pieces))
            def _():
                pass_step(h, late)

    def steps(low, high):
        @pl.loop(low, high)
        def _(i):
            one_step(i)

    @pl.loop(0, pieces)
    def _(k):
        for h in range(2):
            to_mate(h, k).start()

    total_steps = pieces + 2 * gap * (chips - 1)
    steps(0, 3)
    rows = ffn_ref[...]
    gate = jnp.dot(rows, shared_gate_ref[...], preferred_element_type=F32)
    up = jnp.dot(rows, shared_up_ref[...], preferred_element_type=F32)
    hidden = (gate / (1.0 + jnp.exp(-gate)) * up).astype(BF16)
    terms[...] = jnp.dot(hidden, shared_down_ref[...], preferred_element_type=F32).astype(BF16)
    slice_width = s_half.shape[2]

    def columns(j):
        return terms.at[:, pl.ds(pl.multiple_of(j * slice_width, 128), slice_width)]

    second = scatter_sum(
        columns, s_mate, s_half, s_far, (rs_s1, rs_r1, rs_s2, rs_r2),
        (tp, core, partner, chip_at),
    )
    middle = gap * (chips - 1) + 2
    steps(3, middle)
    finish = second()
    steps(middle, total_steps)
    finish()
    shared = s_half[0].astype(F32)
    for d in range(1, chips):
        shared = shared + s_far[d].astype(F32)
    shared_ref[...] = shared

    @pl.loop(0, pieces)
    def _(k):
        for h in range(2):
            to_mate(h, k).wait_send()
            to_partner(h, k).wait()

            @pl.when(stage[h] < chips - 1)
            def _():
                to_ahead(h, k).wait_send()

            @pl.when(stage[h] > 0)
            def _():
                to_back(h, k).wait_send()

    inner_ref[...] = full[...]


def mixed_kernel(
    routed_ref, shared_ref, resid_ref, mixed_ref, back, ep_s, ep_r, *, tp_count, ep_count
):
    tp, ep, chip, core, partner, chip_at, ep_at = places(tp_count, ep_count)
    barrier = pltpu.get_barrier_semaphore()
    for peer in ep_at[1:]:
        pl.semaphore_signal(barrier, inc=1, device_id={"ep": peer}, device_id_type=MESH_ID)
    pl.semaphore_wait(barrier, ep_count - 1)
    copies = []
    for d in range(1, ep_count):
        copy = remote(routed_ref.at[ep_at[d]], back.at[d], ep_s.at[d], ep_r.at[d], {"ep": ep_at[d]})
        copy.start()
        copies.append(copy)
    total = resid_ref[...].astype(F32) + shared_ref[...] + routed_ref[ep].astype(F32)
    for copy in copies:
        copy.wait()
    for d in range(1, ep_count):
        total = total + back[d].astype(F32)
    mixed_ref[...] = total.astype(BF16)


def local(
    tokens,
    norm_gain,
    ffn_gain,
    w_in,
    decay_rate,
    frequency,
    log_step,
    input_real,
    input_imag,
    readout_real,
    readout_imag,
    skip_gain,
    state_real,
    state_imag,
    w_out,
    shared_gate,
    shared_up,
    shared_down,
    expert_gate,
    expert_up,
    expert_down,
    routing,
    route_weight,
):
    seq_count, model_width = tokens.shape
    tp_count = lax.axis_size("tp")
    ep_count = lax.axis_size("ep")
    chips = tp_count // 2
    slice_width = model_width // tp_count
    groups = log_step.shape[0]
    modes = decay_rate.shape[0]
    expert_dev, _, hidden = expert_gate.shape
    expert_count = expert_dev * ep_count
    top_count = routing.shape[1]
    capacity = 2 * seq_count * top_count // expert_count
    slots = ep_count * capacity
    slot_count = expert_dev * slots
    dma = pltpu.SemaphoreType.DMA
    tp_sems = [dma((chips,))] * 4
    local_params = pltpu.CompilerParams(vmem_limit_bytes=VMEM_LIMIT)

    def talk(number, mib):
        return pltpu.CompilerParams(
            collective_id=number, has_side_effects=True, vmem_limit_bytes=mib * 1024 * 1024
        )

    terms, new_real, new_imag, meta = pl.pallas_call(
        functools.partial(mixer_kernel, groups=groups, experts=expert_count, cap=capacity),
        out_shape=(
            jax.ShapeDtypeStruct((seq_count, model_width), BF16),
            jax.ShapeDtypeStruct((seq_count, modes), F32),
            jax.ShapeDtypeStruct((seq_count, modes), F32),
            jax.ShapeDtypeStruct((2 * top_count, seq_count), F32),
        ),
        in_specs=[IN_VMEM] * 16,
        out_specs=(IN_VMEM,) * 4,
        compiler_params=local_params,
        name="mixer",
    )(
        tokens,
        norm_gain[None, :],
        w_in,
        decay_rate[None, :],
        frequency[None, :],
        log_step[None, :],
        input_real,
        input_imag,
        readout_real,
        readout_imag,
        skip_gain[None, :],
        state_real,
        state_imag,
        w_out,
        routing.T,
        route_weight.T,
    )
    block = (seq_count, slice_width)
    ffn_rows, resid_own, rows_all, flat_meta = pl.pallas_call(
        functools.partial(
            resid_kernel, tp_count=tp_count, ep_count=ep_count, first_step=expert_dev * capacity
        ),
        out_shape=(
            jax.ShapeDtypeStruct((seq_count, model_width), BF16),
            jax.ShapeDtypeStruct(block, BF16),
            jax.ShapeDtypeStruct((ep_count,) + block, BF16),
            jax.ShapeDtypeStruct((meta.shape[0], ep_count * seq_count), F32),
        ),
        in_specs=[IN_VMEM] * 4,
        out_specs=(IN_VMEM,) * 4,
        scratch_shapes=[
            pltpu.VMEM((chips,) + block, BF16),
            pltpu.VMEM((chips,) + block, BF16),
            pltpu.VMEM((chips,) + block, BF16),
            pltpu.VMEM((seq_count, model_width), BF16),
            pltpu.VMEM((ep_count,) + block, BF16),
            pltpu.VMEM((ep_count,) + meta.shape, F32),
        ]
        + tp_sems
        + tp_sems
        + [dma((ep_count,))] * 4,
        compiler_params=talk(1, 12),
        name="resid",
    )(terms, tokens, ffn_gain[None, :], meta)

    whole = lambda shape: pl.BlockSpec(shape, lambda e: (0,) * len(shape))
    parts = pl.pallas_call(
        functools.partial(up_kernel, top=top_count, cap=capacity, seqs=seq_count, width=hidden),
        out_shape=jax.ShapeDtypeStruct((slot_count, 2 * hidden), BF16),
        grid=(expert_dev,),
        in_specs=[
            whole(flat_meta.shape),
            whole((ep_count * seq_count, slice_width)),
            pl.BlockSpec((1, slice_width, hidden), lambda e: (e, 0, 0)),
            pl.BlockSpec((1, slice_width, hidden), lambda e: (e, 0, 0)),
        ],
        out_specs=pl.BlockSpec((slots, 2 * hidden), lambda e: (e, 0)),
        compiler_params=local_params,
        name="gate_up",
    )(flat_meta, rows_all.reshape(ep_count * seq_count, slice_width), expert_gate, expert_up)

    pieces = min(8, slot_count // 64)
    piece = slot_count // (4 * pieces)
    steps_wide = (2, pieces, piece, 2 * hidden)
    inner, shared_own = pl.pallas_call(
        functools.partial(inner_kernel, tp_count=tp_count, ep_count=ep_count),
        out_shape=(
            jax.ShapeDtypeStruct((2, 2, pieces, piece, hidden), BF16),
            jax.ShapeDtypeStruct(block, F32),
        ),
        in_specs=[IN_VMEM] * 5,
        out_specs=(IN_VMEM,) * 2,
        scratch_shapes=[pltpu.VMEM(steps_wide, BF16)] * 3
        + [
            pltpu.VMEM((2, 2, pieces, piece, hidden), BF16),
            pltpu.VMEM((seq_count, model_width), BF16),
        ]
        + [pltpu.VMEM((chips,) + block, BF16)] * 3
        + [dma((2, pieces))] * 8
        + tp_sems,
        compiler_params=talk(2, 20),
        name="inner",
    )(
        parts.reshape(2, 2, pieces, piece, 2 * hidden),
        ffn_rows,
        shared_gate,
        shared_up,
        shared_down,
    )

    routed = pl.pallas_call(
        functools.partial(down_kernel, top=top_count, cap=capacity, seqs=seq_count),
        out_shape=jax.ShapeDtypeStruct((ep_count * seq_count, slice_width), BF16),
        grid=(expert_dev,),
        in_specs=[
            whole(flat_meta.shape),
            pl.BlockSpec((slots, hidden), lambda e: (e, 0)),
            pl.BlockSpec((1, hidden, slice_width), lambda e: (e, 0, 0)),
        ],
        out_specs=whole((ep_count * seq_count, slice_width)),
        scratch_shapes=[pltpu.VMEM((ep_count * seq_count, slice_width), F32)],
        compiler_params=local_params,
        name="down",
    )(flat_meta, inner.reshape(slot_count, hidden), expert_down)

    mixed = pl.pallas_call(
        functools.partial(mixed_kernel, tp_count=tp_count, ep_count=ep_count),
        out_shape=jax.ShapeDtypeStruct(block, BF16),
        in_specs=[IN_VMEM] * 3,
        out_specs=IN_VMEM,
        scratch_shapes=[pltpu.VMEM((ep_count,) + block, BF16)] + [dma((ep_count,))] * 2,
        compiler_params=talk(3, 4),
        name="mixed",
    )(routed.reshape((ep_count,) + block), shared_own, resid_own)
    return (mixed, new_real, new_imag)


def solution(mesh):
    placed = (
        P("ep", None),
        P(),
        P(),
        P(None, "tp"),
        P("tp"),
        P("tp"),
        P("tp"),
        P(None, "tp"),
        P(None, "tp"),
        P(None, "tp"),
        P(None, "tp"),
        P("tp"),
        P("ep", "tp"),
        P("ep", "tp"),
        P("tp", None),
        P(None, "tp"),
        P(None, "tp"),
        P("tp", None),
        P("ep", "tp", None),
        P("ep", "tp", None),
        P("ep", None, "tp"),
        P("ep", None),
        P("ep", None),
    )
    return jax.shard_map(
        local,
        mesh=mesh,
        in_specs=placed,
        out_specs=(P("ep", "tp"), P("ep", "tp"), P("ep", "tp")),
        check_vma=False,
    )
```

```python
import functools

import jax
import jax.numpy as jnp
from jax import lax
from jax.experimental import pallas as pl
from jax.experimental.pallas import tpu as pltpu
from jax.sharding import PartitionSpec as P

EPS = 1e-06
ROUTED_SCALE = 2.5
F32 = jnp.float32
BF16 = jnp.bfloat16
VMEM_LIMIT = 20 * 1024 * 1024
MESH_ID = pl.DeviceIdType.MESH
IN_VMEM = pl.BlockSpec(memory_space=pltpu.VMEM)


def shift_of(size):
    assert size & (size - 1) == 0
    return size.bit_length() - 1


def split_index(shape, axis, size):
    places = lax.broadcasted_iota(jnp.int32, shape, axis)
    return lax.shift_right_logical(places, shift_of(size))


def mixer_kernel(
    tokens_ref,
    gain_ref,
    w_in_ref,
    decay_ref,
    freq_ref,
    logstep_ref,
    in_re_ref,
    in_im_ref,
    out_re_ref,
    out_im_ref,
    skip_ref,
    old_re_ref,
    old_im_ref,
    w_out_ref,
    ids_ref,
    share_ref,
    terms_ref,
    new_re_ref,
    new_im_ref,
    meta_ref,
    *,
    groups,
    experts,
    cap,
):
    top, seqs = ids_ref.shape
    square = (seqs, seqs)
    before = (
        lax.broadcasted_iota(jnp.int32, square, 0) < lax.broadcasted_iota(jnp.int32, square, 1)
    ).astype(BF16)
    named = lax.broadcasted_iota(jnp.int32, (experts, seqs), 0)
    taken = jnp.zeros((experts, 1), F32)
    shares = share_ref[...]
    scale = ROUTED_SCALE / jnp.sum(shares, axis=0, keepdims=True)
    for k in range(top):
        ids = ids_ref[k : k + 1, :]
        hot = (named == ids).astype(F32)
        earlier = jnp.dot(hot.astype(BF16), before, preferred_element_type=F32) + taken
        rank = jnp.sum(earlier * hot, axis=0, keepdims=True)
        taken = taken + jnp.sum(hot, axis=1, keepdims=True)
        meta_ref[k : k + 1, :] = (ids * cap).astype(F32) + rank
        meta_ref[top + k : top + k + 1, :] = shares[k : k + 1, :] * scale
    tokens = tokens_ref[...].astype(F32)
    factor = lax.rsqrt(jnp.mean(tokens * tokens, axis=-1, keepdims=True) + EPS)
    normed = (tokens * factor * gain_ref[...]).astype(BF16)
    drive = jnp.dot(normed, w_in_ref[...], preferred_element_type=F32).astype(BF16)
    chan = in_re_ref.shape[0]
    width = decay_ref.shape[1] // groups
    wide = (groups * chan, groups * width)
    own_group = split_index(wide, 0, chan) == split_index(wide, 1, width)

    def spread(ref):
        tiled = jnp.concatenate([ref[...]] * groups, axis=0)
        return jnp.where(own_group, tiled, 0.0).astype(BF16)

    decay, freq = decay_ref[...], freq_ref[...]
    over = (groups, groups * width)
    member = lax.broadcasted_iota(jnp.int32, over, 0) == split_index(over, 1, width)
    column = jnp.sum(jnp.where(
        lax.broadcasted_iota(jnp.int32, (groups, groups), 0)
        == lax.broadcasted_iota(jnp.int32, (groups, groups), 1), logstep_ref[...], 0.0,
    ), axis=1, keepdims=True)
    step = jnp.exp(jnp.sum(jnp.where(member, column, 0.0), axis=0, keepdims=True))
    mag = jnp.exp(-decay * step)
    pole_re = mag * jnp.cos(freq * step)
    pole_im = mag * jnp.sin(freq * step)
    norm = decay * decay + freq * freq
    diff = pole_re - 1.0
    lift_re = (-decay * diff + freq * pole_im) / norm
    lift_im = (-decay * pole_im - freq * diff) / norm
    push_re = jnp.dot(drive, spread(in_re_ref), preferred_element_type=F32)
    push_im = jnp.dot(drive, spread(in_im_ref), preferred_element_type=F32)
    old_re, old_im = old_re_ref[...], old_im_ref[...]
    new_re = pole_re * old_re - pole_im * old_im + lift_re * push_re - lift_im * push_im
    new_im = pole_re * old_im + pole_im * old_re + lift_re * push_im + lift_im * push_re
    new_re_ref[...] = new_re
    new_im_ref[...] = new_im
    nt = (((1,), (1,)), ((), ()))
    read = lax.dot_general(
        new_re.astype(BF16), spread(out_re_ref), nt, preferred_element_type=F32
    ) - lax.dot_general(new_im.astype(BF16), spread(out_im_ref), nt, preferred_element_type=F32)
    read = read + skip_ref[...] * drive.astype(F32)
    activated = jax.nn.gelu(read).astype(BF16)
    terms_ref[...] = jnp.dot(activated, w_out_ref[...], preferred_element_type=F32).astype(BF16)


def enter(tp, ep, partner, same_core, ep_peers):
    barrier = pltpu.get_barrier_semaphore()
    peers = [{"tp": d} for d in [partner] + same_core] + [{"ep": d} for d in ep_peers]
    for peer in peers:
        pl.semaphore_signal(barrier, inc=1, device_id=peer, device_id_type=MESH_ID)
    pl.semaphore_wait(barrier, len(peers))


def remote(src, dst, send_sem, recv_sem, peer):
    return pltpu.make_async_remote_copy(
        src_ref=src,
        dst_ref=dst,
        send_sem=send_sem,
        recv_sem=recv_sem,
        device_id=peer,
        device_id_type=MESH_ID,
    )


def places(tp_count, ep_count):
    tp, ep = lax.axis_index("tp"), lax.axis_index("ep")
    chips = tp_count // 2
    chip, core = tp // 2, tp % 2
    partner = chip * 2 + (1 - core)
    chip_at = [(chip + d) % chips for d in range(chips)]
    ep_at = [(ep + d) % ep_count for d in range(ep_count)]
    return tp, ep, chip, core, partner, chip_at, ep_at


def scatter_sum(block_of, mate, half, far, sems, where):
    tp, core, partner, chip_at = where
    s1, r1, s2, r2 = sems
    chips = len(chip_at)
    order = list(range(1, chips)) + [0]
    first = {}
    for d in order:
        first[d] = remote(
            block_of(chip_at[d] * 2 + (1 - core)),
            mate.at[d],
            s1.at[d],
            r1.at[d],
            {"tp": partner},
        )
        first[d].start()
    second = {}
    return functools.partial(scatter_second, block_of, mate, half, far, sems, where, first, second)


def scatter_second(block_of, mate, half, far, sems, where, first, second):
    tp, core, partner, chip_at = where
    s1, r1, s2, r2 = sems
    chips = len(chip_at)
    order = list(range(1, chips)) + [0]
    for d in order:
        first[d].wait_recv()
        own = block_of(chip_at[d] * 2 + core)[...].astype(F32) + mate[d].astype(F32)
        half[d] = own.astype(BF16)
        if d:
            second[d] = remote(
                half.at[d], far.at[d], s2.at[d], r2.at[d], {"tp": chip_at[d] * 2 + core}
            )
            second[d].start()

    def finish():
        for d in order:
            first[d].wait_send()
        for d in range(1, chips):
            second[d].wait()

    return finish


def gather_start(own, store, sems, where):
    tp, core, partner, chip_at = where
    s1, r1, s2, r2 = sems
    chips = len(chip_at)
    sends = []
    for d in range(1, chips):
        copy = remote(own, store(tp), s1.at[d], r1.at[d], {"tp": chip_at[d] * 2 + core})
        copy.start()
        sends.append(copy)
    mine = remote(own, store(tp), s2.at[0], r2.at[0], {"tp": partner})
    mine.start()

    def finish():
        passed = [mine]
        for d in range(1, chips):
            sends[d - 1].wait_recv()
            source = chip_at[chips - d] * 2 + core
            onward = remote(store(source), store(source), s2.at[d], r2.at[d], {"tp": partner})
            onward.start()
            passed.append(onward)
        for copy in sends:
            copy.wait_send()
        for copy in passed:
            copy.wait()

    return finish


def resid_kernel(
    terms_ref,
    tokens_ref,
    gain_ref,
    meta_ref,
    ffn_ref,
    resid_ref,
    rows_ref,
    metas_ref,
    mate,
    half,
    far,
    full,
    rows,
    metas,
    rs_s1,
    rs_r1,
    rs_s2,
    rs_r2,
    ag_s1,
    ag_r1,
    ag_s2,
    ag_r2,
    ep_s,
    ep_r,
    meta_s,
    meta_r,
    *,
    tp_count,
    ep_count,
    first_step,
):
    tp, ep, chip, core, partner, chip_at, ep_at = places(tp_count, ep_count)
    enter(tp, ep, partner, [c * 2 + core for c in chip_at[1:]], ep_at[1:])
    where = (tp, core, partner, chip_at)
    slice_width = rows.shape[2]

    def columns(ref):
        return lambda j: ref.at[:, pl.ds(pl.multiple_of(j * slice_width, 128), slice_width)]

    meta_copies = []
    for d in range(1, ep_count):
        copy = remote(meta_ref, metas.at[ep], meta_s.at[d], meta_r.at[d], {"ep": ep_at[d]})
        copy.start()
        meta_copies.append(copy)
    scatter_sum(columns(terms_ref), mate, half, far, (rs_s1, rs_r1, rs_s2, rs_r2), where)()()
    total = half[0].astype(F32)
    for d in range(1, len(chip_at)):
        total = total + far[d].astype(F32)
    resid = (columns(tokens_ref)(tp)[...].astype(F32) + total).astype(BF16)
    resid_ref[...] = resid
    columns(full)(tp)[...] = resid
    gather_start(columns(full)(tp), columns(full), (ag_s1, ag_r1, ag_s2, ag_r2), where)()
    whole = full[...].astype(F32)
    factor = lax.rsqrt(jnp.mean(whole * whole, axis=-1, keepdims=True) + EPS)
    gain_own = columns(gain_ref)(tp)[...]
    rows[ep] = (resid.astype(F32) * factor * gain_own).astype(BF16)
    row_copies = []
    for d in range(1, ep_count):
        copy = remote(rows.at[ep], rows.at[ep], ep_s.at[d], ep_r.at[d], {"ep": ep_at[d]})
        copy.start()
        row_copies.append(copy)
    ffn_ref[...] = (whole * factor * gain_ref[...]).astype(BF16)
    metas[ep] = meta_ref[...]
    for copy in meta_copies + row_copies:
        copy.wait()
    rows_ref[...] = rows[...]
    flat = jnp.concatenate([metas[b] for b in range(ep_count)], axis=1)
    base = (ep * first_step).astype(F32)
    row = lax.broadcasted_iota(jnp.int32, flat.shape, 0)
    metas_ref[...] = flat - jnp.where(row < flat.shape[0] // 2, base, 0.0)


def slot_map(meta_ref, row, block, base, slots, cap, seqs, values):
    shape = (slots, meta_ref.shape[1])
    slot = lax.broadcasted_iota(jnp.int32, shape, 0)
    same = lax.shift_right_logical(slot, shift_of(cap)) == split_index(shape, 1, seqs)
    wanted = ((slot & (cap - 1)) + base).astype(F32)
    total = jnp.zeros(shape, F32)
    for k in range(row):
        total = total + jnp.where(meta_ref[k : k + 1, :] == wanted, values(k), 0.0)
    return jnp.where(same, total, 0.0)


def up_kernel(meta_ref, rows_ref, gate_ref, up_ref, out_ref, *, top, cap, seqs, width):
    base = pl.program_id(0) * cap
    slots = out_ref.shape[0]
    chosen = slot_map(meta_ref, top, 0, base, slots, cap, seqs, lambda k: 1.0).astype(BF16)
    picked = jnp.dot(chosen, rows_ref[...], preferred_element_type=F32).astype(BF16)
    out_ref[:, :width] = jnp.dot(picked, gate_ref[0], preferred_element_type=F32).astype(BF16)
    out_ref[:, width:] = jnp.dot(picked, up_ref[0], preferred_element_type=F32).astype(BF16)


def down_kernel(meta_ref, inner_ref, down_ref, out_ref, total, *, top, cap, seqs):
    expert = pl.program_id(0)
    slots = inner_ref.shape[0]
    mix = slot_map(
        meta_ref, top, 0, expert * cap, slots, cap, seqs, lambda k: meta_ref[top + k : top + k + 1, :]
    ).astype(BF16)
    terms = jnp.dot(inner_ref[...], down_ref[0], preferred_element_type=F32).astype(BF16)
    part = lax.dot_general(mix, terms, (((0,), (0,)), ((), ())), preferred_element_type=F32)

    @pl.when(expert == 0)
    def _():
        total[...] = part

    @pl.when(expert > 0)
    def _():
        total[...] += part

    out_ref[...] = total[...].astype(BF16)


def inner_kernel(
    parts_ref,
    ffn_ref,
    shared_gate_ref,
    shared_up_ref,
    shared_down_ref,
    inner_ref,
    shared_ref,
    mate,
    inbox,
    outbox,
    full,
    terms,
    s_mate,
    s_half,
    s_far,
    m_s,
    m_r,
    c_s,
    c_r,
    g_s,
    g_r,
    p_s,
    p_r,
    rs_s1,
    rs_r1,
    rs_s2,
    rs_r2,
    *,
    tp_count,
    ep_count,
):
    tp, ep, chip, core, partner, chip_at, ep_at = places(tp_count, ep_count)
    chips = tp_count // 2
    pieces = full.shape[2]
    width = full.shape[4]
    other = 1 - core
    enter(tp, ep, partner, [c * 2 + core for c in chip_at[1:]], [])
    stage = [chips - 1 - chip, chip]
    ahead = [(chip - 1) * 2 + core, (chip + 1) * 2 + core]
    back = [(chip + 1) * 2 + core, (chip - 1) * 2 + core]

    def to_mate(h, k):
        return remote(
            parts_ref.at[h, other, k], mate.at[h, k], m_s.at[h, k], m_r.at[h, k], {"tp": partner}
        )

    def to_ahead(h, k):
        return remote(
            outbox.at[h, k], inbox.at[h, k], c_s.at[h, k], c_r.at[h, k], {"tp": ahead[h]}
        )

    def to_back(h, k):
        piece = full.at[h, core, k]
        return remote(piece, piece, g_s.at[h, k], g_r.at[h, k], {"tp": back[h]})

    def to_partner(h, k):
        piece = full.at[h, core, k]
        return remote(piece, piece, p_s.at[h, k], p_r.at[h, k], {"tp": partner})

    def sum_step(h, k):
        to_mate(h, k).wait_recv()
        own = parts_ref[h, core, k].astype(F32) + mate[h, k].astype(F32)

        @pl.when(stage[h] == 0)
        def _():
            outbox[h, k] = own.astype(BF16)

        @pl.when(stage[h] > 0)
        def _():
            to_ahead(h, k).wait_recv()
            total = own + inbox[h, k].astype(F32)

            @pl.when(stage[h] < chips - 1)
            def _():
                outbox[h, k] = total.astype(BF16)

            @pl.when(stage[h] == chips - 1)
            def _():
                gate, up = total[:, :width], total[:, width:]
                full[h, core, k] = (gate / (1.0 + jnp.exp(-gate)) * up).astype(BF16)
                to_back(h, k).start()
                to_partner(h, k).start()

        @pl.when(stage[h] < chips - 1)
        def _():
            to_ahead(h, k).start()

    def pass_step(h, k):
        to_back(h, k).wait_recv()

        @pl.when(stage[h] > 0)
        def _():
            to_back(h, k).start()

        to_partner(h, k).start()

    gap, gap_back = 3, 2

    def one_step(i):
        for h in range(2):
            k = i - gap * stage[h]

            @pl.when((k >= 0) & (k < pieces))
            def _():
                sum_step(h, k)

        for h in range(2):
            late = i - gap * (chips - 1) - gap_back * (chips - 1 - stage[h])

            @pl.when((stage[h] < chips - 1) & (late >= 0) & (late < pieces))
            def _():
                pass_step(h, late)

    def steps(low, high):
        @pl.loop(low, high)
        def _(i):
            one_step(i)

    @pl.loop(0, pieces)
    def _(k):
        for h in range(2):
            to_mate(h, k).start()

    total_steps = pieces + (gap + gap_back) * (chips - 1)
    steps(0, 3)
    rows = ffn_ref[...]
    gate = jnp.dot(rows, shared_gate_ref[...], preferred_element_type=F32)
    up = jnp.dot(rows, shared_up_ref[...], preferred_element_type=F32)
    hidden = (gate / (1.0 + jnp.exp(-gate)) * up).astype(BF16)
    terms[...] = jnp.dot(hidden, shared_down_ref[...], preferred_element_type=F32).astype(BF16)
    slice_width = s_half.shape[2]

    def columns(j):
        return terms.at[:, pl.ds(pl.multiple_of(j * slice_width, 128), slice_width)]

    second = scatter_sum(
        columns, s_mate, s_half, s_far, (rs_s1, rs_r1, rs_s2, rs_r2),
        (tp, core, partner, chip_at),
    )
    middle = gap * (chips - 1) + 2
    steps(3, middle)
    finish = second()
    steps(middle, total_steps)
    finish()
    shared = s_half[0].astype(F32)
    for d in range(1, chips):
        shared = shared + s_far[d].astype(F32)
    shared_ref[...] = shared

    @pl.loop(0, pieces)
    def _(k):
        for h in range(2):
            to_mate(h, k).wait_send()
            to_partner(h, k).wait()

            @pl.when(stage[h] < chips - 1)
            def _():
                to_ahead(h, k).wait_send()

            @pl.when(stage[h] > 0)
            def _():
                to_back(h, k).wait_send()

    inner_ref[...] = full[...]


def mixed_kernel(
    routed_ref, shared_ref, resid_ref, mixed_ref, back, ep_s, ep_r, *, tp_count, ep_count
):
    tp, ep, chip, core, partner, chip_at, ep_at = places(tp_count, ep_count)
    barrier = pltpu.get_barrier_semaphore()
    for peer in ep_at[1:]:
        pl.semaphore_signal(barrier, inc=1, device_id={"ep": peer}, device_id_type=MESH_ID)
    pl.semaphore_wait(barrier, ep_count - 1)
    copies = []
    for d in range(1, ep_count):
        copy = remote(routed_ref.at[ep_at[d]], back.at[d], ep_s.at[d], ep_r.at[d], {"ep": ep_at[d]})
        copy.start()
        copies.append(copy)
    total = resid_ref[...].astype(F32) + shared_ref[...] + routed_ref[ep].astype(F32)
    for copy in copies:
        copy.wait()
    for d in range(1, ep_count):
        total = total + back[d].astype(F32)
    mixed_ref[...] = total.astype(BF16)


def local(
    tokens,
    norm_gain,
    ffn_gain,
    w_in,
    decay_rate,
    frequency,
    log_step,
    input_real,
    input_imag,
    readout_real,
    readout_imag,
    skip_gain,
    state_real,
    state_imag,
    w_out,
    shared_gate,
    shared_up,
    shared_down,
    expert_gate,
    expert_up,
    expert_down,
    routing,
    route_weight,
):
    seq_count, model_width = tokens.shape
    tp_count = lax.axis_size("tp")
    ep_count = lax.axis_size("ep")
    chips = tp_count // 2
    slice_width = model_width // tp_count
    groups = log_step.shape[0]
    modes = decay_rate.shape[0]
    expert_dev, _, hidden = expert_gate.shape
    expert_count = expert_dev * ep_count
    top_count = routing.shape[1]
    capacity = 2 * seq_count * top_count // expert_count
    slots = ep_count * capacity
    slot_count = expert_dev * slots
    dma = pltpu.SemaphoreType.DMA
    tp_sems = [dma((chips,))] * 4
    local_params = pltpu.CompilerParams(vmem_limit_bytes=VMEM_LIMIT)

    def talk(number, mib):
        return pltpu.CompilerParams(
            collective_id=number, has_side_effects=True, vmem_limit_bytes=mib * 1024 * 1024
        )

    terms, new_real, new_imag, meta = pl.pallas_call(
        functools.partial(mixer_kernel, groups=groups, experts=expert_count, cap=capacity),
        out_shape=(
            jax.ShapeDtypeStruct((seq_count, model_width), BF16),
            jax.ShapeDtypeStruct((seq_count, modes), F32),
            jax.ShapeDtypeStruct((seq_count, modes), F32),
            jax.ShapeDtypeStruct((2 * top_count, seq_count), F32),
        ),
        in_specs=[IN_VMEM] * 16,
        out_specs=(IN_VMEM,) * 4,
        compiler_params=pltpu.CompilerParams(vmem_limit_bytes=3 * VMEM_LIMIT),
        name="mixer",
    )(
        tokens,
        norm_gain[None, :],
        w_in,
        decay_rate[None, :],
        frequency[None, :],
        log_step[None, :],
        input_real,
        input_imag,
        readout_real,
        readout_imag,
        skip_gain[None, :],
        state_real,
        state_imag,
        w_out,
        routing.T,
        route_weight.T,
    )
    block = (seq_count, slice_width)
    ffn_rows, resid_own, rows_all, flat_meta = pl.pallas_call(
        functools.partial(
            resid_kernel, tp_count=tp_count, ep_count=ep_count, first_step=expert_dev * capacity
        ),
        out_shape=(
            jax.ShapeDtypeStruct((seq_count, model_width), BF16),
            jax.ShapeDtypeStruct(block, BF16),
            jax.ShapeDtypeStruct((ep_count,) + block, BF16),
            jax.ShapeDtypeStruct((meta.shape[0], ep_count * seq_count), F32),
        ),
        in_specs=[IN_VMEM] * 4,
        out_specs=(IN_VMEM,) * 4,
        scratch_shapes=[
            pltpu.VMEM((chips,) + block, BF16),
            pltpu.VMEM((chips,) + block, BF16),
            pltpu.VMEM((chips,) + block, BF16),
            pltpu.VMEM((seq_count, model_width), BF16),
            pltpu.VMEM((ep_count,) + block, BF16),
            pltpu.VMEM((ep_count,) + meta.shape, F32),
        ]
        + tp_sems
        + tp_sems
        + [dma((ep_count,))] * 4,
        compiler_params=talk(1, 12),
        name="resid",
    )(terms, tokens, ffn_gain[None, :], meta)

    whole = lambda shape: pl.BlockSpec(shape, lambda e: (0,) * len(shape))
    parts = pl.pallas_call(
        functools.partial(up_kernel, top=top_count, cap=capacity, seqs=seq_count, width=hidden),
        out_shape=jax.ShapeDtypeStruct((slot_count, 2 * hidden), BF16),
        grid=(expert_dev,),
        in_specs=[
            whole(flat_meta.shape),
            whole((ep_count * seq_count, slice_width)),
            pl.BlockSpec((1, slice_width, hidden), lambda e: (e, 0, 0)),
            pl.BlockSpec((1, slice_width, hidden), lambda e: (e, 0, 0)),
        ],
        out_specs=pl.BlockSpec((slots, 2 * hidden), lambda e: (e, 0)),
        compiler_params=local_params,
        name="gate_up",
    )(flat_meta, rows_all.reshape(ep_count * seq_count, slice_width), expert_gate, expert_up)

    pieces = min(8, slot_count // 64)
    piece = slot_count // (4 * pieces)
    steps_wide = (2, pieces, piece, 2 * hidden)
    inner, shared_own = pl.pallas_call(
        functools.partial(inner_kernel, tp_count=tp_count, ep_count=ep_count),
        out_shape=(
            jax.ShapeDtypeStruct((2, 2, pieces, piece, hidden), BF16),
            jax.ShapeDtypeStruct(block, F32),
        ),
        in_specs=[IN_VMEM] * 5,
        out_specs=(IN_VMEM,) * 2,
        scratch_shapes=[pltpu.VMEM(steps_wide, BF16)] * 3
        + [
            pltpu.VMEM((2, 2, pieces, piece, hidden), BF16),
            pltpu.VMEM((seq_count, model_width), BF16),
        ]
        + [pltpu.VMEM((chips,) + block, BF16)] * 3
        + [dma((2, pieces))] * 8
        + tp_sems,
        compiler_params=talk(2, 20),
        name="inner",
    )(
        parts.reshape(2, 2, pieces, piece, 2 * hidden),
        ffn_rows,
        shared_gate,
        shared_up,
        shared_down,
    )

    routed = pl.pallas_call(
        functools.partial(down_kernel, top=top_count, cap=capacity, seqs=seq_count),
        out_shape=jax.ShapeDtypeStruct((ep_count * seq_count, slice_width), BF16),
        grid=(expert_dev,),
        in_specs=[
            whole(flat_meta.shape),
            pl.BlockSpec((slots, hidden), lambda e: (e, 0)),
            pl.BlockSpec((1, hidden, slice_width), lambda e: (e, 0, 0)),
        ],
        out_specs=whole((ep_count * seq_count, slice_width)),
        scratch_shapes=[pltpu.VMEM((ep_count * seq_count, slice_width), F32)],
        compiler_params=local_params,
        name="down",
    )(flat_meta, inner.reshape(slot_count, hidden), expert_down)

    mixed = pl.pallas_call(
        functools.partial(mixed_kernel, tp_count=tp_count, ep_count=ep_count),
        out_shape=jax.ShapeDtypeStruct(block, BF16),
        in_specs=[IN_VMEM] * 3,
        out_specs=IN_VMEM,
        scratch_shapes=[pltpu.VMEM((ep_count,) + block, BF16)] + [dma((ep_count,))] * 2,
        compiler_params=talk(3, 4),
        name="mixed",
    )(routed.reshape((ep_count,) + block), shared_own, resid_own)
    return (mixed, new_real, new_imag)


def solution(mesh):
    placed = (
        P("ep", None),
        P(),
        P(),
        P(None, "tp"),
        P("tp"),
        P("tp"),
        P("tp"),
        P(None, "tp"),
        P(None, "tp"),
        P(None, "tp"),
        P(None, "tp"),
        P("tp"),
        P("ep", "tp"),
        P("ep", "tp"),
        P("tp", None),
        P(None, "tp"),
        P(None, "tp"),
        P("tp", None),
        P("ep", "tp", None),
        P("ep", "tp", None),
        P("ep", None, "tp"),
        P("ep", None),
        P("ep", None),
    )
    return jax.shard_map(
        local,
        mesh=mesh,
        in_specs=placed,
        out_specs=(P("ep", "tp"), P("ep", "tp"), P("ep", "tp")),
        check_vma=False,
    )
```
